32 devices in a mesh: sp: 4 (over z), dp: 8 (over y, x, core).
Axes of the slice: x: 2, y: 2, z: 4, core: 2. Of those that a mesh axis runs over, the one named last changes fastest.
Arguments:
- probe_vectors: bfloat16 [4096, 1024], P(('dp', 'sp')), may hold values from -6 to 6
- address_vectors: bfloat16 [4096, 1024], P(('dp', 'sp')), may hold values from -6 to 6
- content_vectors: bfloat16 [4096, 2048], P(('dp', 'sp')), may hold values from -6 to 6
- adjoint_of_result: bfloat16 [4096, 2048], P(('dp', 'sp')), may hold values from -0.5 to 0.5
- compact_factor: bfloat16 [4096, 64], P(('dp', 'sp')), may hold values from -7.5 to 7.5
- latent_to_damping_map: bfloat16 [64, 1024], replicated, may hold values from -0.75 to 0.75
- damping_shift_term: float32 [1024], replicated
- surplus_damping: bfloat16 [4096, 16], P(('dp', 'sp')), may hold values from -0.7 to 0
Outputs:
- query_grad: bfloat16 [4096, 1024], P(('dp', 'sp'))
- key_grad: bfloat16 [4096, 1024], P(('dp', 'sp'))
- value_grad: bfloat16 [4096, 2048], P(('dp', 'sp'))
- latent_grad: bfloat16 [4096, 64], P(('dp', 'sp'))
- weight_grad: float32 [64, 1024], replicated
The draws below stay inside these ranges and needn't reach their ends.
All inputs are finite; a program needn't handle non-finite values.
Results may differ from the reference program's by a relative error of at most 0.005.
Values may be sent and summed in bfloat16 or wider, within the bound.
A program may use at most 64 MiB of HBM per device.

```python
import math
import jax
import jax.numpy as jnp
from jax import lax

HEADS = 16
KEY_CHANNELS = 64
VALUE_DIM = 128
RANK = 64
BLOCK = 64
SEQ = 512
TOKENS = 4096
N_DP = 8


def draw_compact_factor(key, part):
    base_key = jax.random.fold_in(key, 11)
    scale_key = jax.random.fold_in(key, 12)
    factor = jnp.exp(jax.random.uniform(scale_key, (TOKENS // BLOCK, 1), jnp.float32, math.log(0.5), math.log(1.5)))
    factor = jnp.repeat(factor, BLOCK, axis=0)
    noise = jnp.clip(jax.random.normal(base_key, (TOKENS, RANK), jnp.float32), -5.0, 5.0)
    return (noise * factor).astype(jnp.bfloat16)


def draw_damping_shift_term(key, part):
    pick_key = jax.random.fold_in(key, 21)
    mixed_key = jax.random.fold_in(key, 22)
    slow_key = jax.random.fold_in(key, 23)
    mixed_count = HEADS // 2
    jitter = 0.5
    ranking = jax.random.permutation(pick_key, HEADS)
    mixed = (ranking < mixed_count)[:, None]
    mixed_value = jax.random.uniform(mixed_key, (HEADS, KEY_CHANNELS), jnp.float32, -3.0, 6.0)
    slow_value = math.log(SEQ / 16.0) + 1.2 + jax.random.uniform(slow_key, (HEADS, KEY_CHANNELS), jnp.float32, -jitter, jitter)
    return jnp.where(mixed, mixed_value, slow_value).reshape(HEADS * KEY_CHANNELS)


def draw_surplus_damping(key, part):
    where_key = jax.random.fold_in(key, 31)
    depth_key = jax.random.fold_in(key, 32)
    hits = jax.random.uniform(where_key, (TOKENS, HEADS), jnp.float32) < 2.0 / SEQ
    depth = jax.random.uniform(depth_key, (TOKENS, HEADS), jnp.float32, math.log(0.5), math.log(0.8))
    return jnp.where(hits, depth, jnp.zeros_like(depth)).astype(jnp.bfloat16)


def level_of(stream_key, dims, pieces, smallest, top_value):
    loudness = 1.0
    for dim, blocks in pieces:
        heights = jax.random.uniform(jax.random.fold_in(jax.random.fold_in(stream_key, 6), dim), (blocks,), jnp.float32, smallest / len(pieces), top_value / len(pieces))
        loudness = loudness * jnp.repeat(jnp.exp(heights), dims[dim] // blocks).reshape((-1,) + (1,) * (len(dims) - 1 - dim))
    return loudness


def centred(key, dims, spread, reach, shards=(), kind=jnp.bfloat16):
    result = jax.random.normal(key, dims, jnp.float32) * spread
    if len(shards) > 0:
        result = level_of(key, dims, shards, -0.22, 0.18) * result
    return jnp.clip(result, min=-reach, max=reach).astype(kind)


def setup_inputs(seed: int = 0) -> dict:
    splits = jax.random.split(jax.random.key(seed), 9)
    probe_vectors = centred(splits[0], (TOKENS, HEADS * KEY_CHANNELS), 1.0, 6.0, ((0, 32),))
    address_vectors = centred(splits[1], (TOKENS, HEADS * KEY_CHANNELS), 1.0, 6.0, ((0, 32),))
    content_vectors = centred(splits[2], (TOKENS, HEADS * VALUE_DIM), 1.0, 6.0, ((0, 32),))
    adjoint_of_result = centred(splits[3], (TOKENS, HEADS * VALUE_DIM), (8 * (SEQ * VALUE_DIM) ** -0.5), 0.5, ((0, 32),))
    compact_factor = draw_compact_factor(jax.random.fold_in(splits[8], 71), 0)
    latent_to_damping_map = centred(splits[5], (RANK, HEADS * KEY_CHANNELS), RANK ** -0.5, 0.75)
    damping_shift_term = draw_damping_shift_term(jax.random.fold_in(splits[8], 71), 0)
    surplus_damping = draw_surplus_damping(jax.random.fold_in(splits[8], 71), 0)
    return {"probe_vectors": probe_vectors, "address_vectors": address_vectors, "content_vectors": content_vectors, "adjoint_of_result": adjoint_of_result, "compact_factor": compact_factor, "latent_to_damping_map": latent_to_damping_map, "damping_shift_term": damping_shift_term, "surplus_damping": surplus_damping}


gate_norm = 16.0
highest = lax.Precision.HIGHEST

def carry_states(block_total, increments):
    log_totals = block_total[:, :, 0, :]
    running = jnp.cumsum(log_totals, axis=1)
    before = running - log_totals
    blocks = log_totals.shape[1]
    order = jnp.arange(blocks, dtype=jnp.int32)
    earlier_mask = (order[None, :] < order[:, None])[None, :, :, None]
    exponent = before[:, :, None, :] - running[:, None, :, :]
    exponent = jnp.where(earlier_mask, exponent, jnp.zeros_like(exponent))
    weights = jnp.where(earlier_mask, jnp.exp(exponent), jnp.zeros_like(exponent))
    return jnp.einsum('hnmk,mhkv->nhkv', weights, increments, precision=highest)

def gla_forward(probe_vectors, address_vectors, content_vectors, logarithm_decay):
    head_count, seq_len, key_width = probe_vectors.shape
    value_width = content_vectors.shape[2]
    blocks = seq_len // BLOCK

    def blocked(tensor):
        return tensor.reshape(head_count, blocks, BLOCK, tensor.shape[2])
    cumulative = jnp.cumsum(blocked(logarithm_decay), axis=2)
    block_total = cumulative[:, :, BLOCK - 1:, :]
    keys_block = blocked(address_vectors)
    query_decayed = blocked(probe_vectors) * key_width ** (-0.5) * jnp.exp(cumulative)
    key_inverse = keys_block * jnp.exp(-cumulative)
    key_to_end = keys_block * jnp.exp(block_total - cumulative)
    value_block = blocked(content_vectors)
    scores = jnp.einsum('hnik,hnjk->hnij', query_decayed, key_inverse, precision=highest)
    positions = jnp.arange(BLOCK, dtype=jnp.int32)
    causal = positions[:, None] >= positions[None, :]
    scores = jnp.where(causal, scores, jnp.zeros_like(scores))
    within_block = jnp.einsum('hnij,hnjv->hniv', scores, value_block, precision=highest)
    increments = jnp.einsum('hnjk,hnjv->nhkv', key_to_end, value_block, precision=highest)
    earlier = carry_states(block_total, increments)
    carried = jnp.einsum('hnik,nhkv->hniv', query_decayed, earlier, precision=highest)
    return (within_block + carried).reshape(head_count, seq_len, value_width)

def split_into_heads(tensor, width):
    return tensor.astype(jnp.float32).reshape(SEQ, HEADS, width).transpose(1, 0, 2)

def to_rows(tensor):
    return tensor.transpose(1, 0, 2).reshape(SEQ, tensor.shape[0] * tensor.shape[2])

def stream_array_group(tensor):
    return tensor.reshape(N_DP, SEQ, tensor.shape[1])

def flatten(tensor):
    return tensor.reshape(TOKENS, tensor.shape[2])

def reference(probe_vectors, address_vectors, content_vectors, adjoint_of_result, compact_factor, latent_to_damping_map, damping_shift_term, surplus_damping):

    def lone_stream(input_bundle):
        query_token_rows, key_token_rows, value_token_rows, upstream_rows, hidden_code_rows, spike_rows = input_bundle
        gate_logit = jnp.dot(hidden_code_rows, latent_to_damping_map, preferred_element_type=jnp.float32) + damping_shift_term
        logarithm_decay = split_into_heads(jax.nn.log_sigmoid(gate_logit) / gate_norm, KEY_CHANNELS)
        logarithm_decay = logarithm_decay + spike_rows.astype(jnp.float32).T[:, :, None]
        _, pullback = jax.vjp(gla_forward, split_into_heads(query_token_rows, KEY_CHANNELS), split_into_heads(key_token_rows, KEY_CHANNELS), split_into_heads(value_token_rows, VALUE_DIM), logarithm_decay)
        grad_query, grad_key, grad_value, grad_decay = pullback(split_into_heads(upstream_rows, VALUE_DIM))
        gate_grad = (to_rows(grad_decay) * jax.nn.sigmoid(-gate_logit) / gate_norm).astype(jnp.bfloat16)
        latent_part = jnp.dot(gate_grad, latent_to_damping_map.T, preferred_element_type=jnp.float32).astype(jnp.bfloat16)
        weight_term = jnp.dot(hidden_code_rows.T, gate_grad, preferred_element_type=jnp.float32)
        return (to_rows(grad_query).astype(jnp.bfloat16), to_rows(grad_key).astype(jnp.bfloat16), to_rows(grad_value).astype(jnp.bfloat16), latent_part, weight_term)
    returned_results = lax.map(lone_stream, (stream_array_group(probe_vectors), stream_array_group(address_vectors), stream_array_group(content_vectors), stream_array_group(adjoint_of_result), stream_array_group(compact_factor), stream_array_group(surplus_damping)))
    weight_grad = lax.optimization_barrier(jnp.sum(returned_results[4], axis=0))
    return (flatten(returned_results[0]), flatten(returned_results[1]), flatten(returned_results[2]), flatten(returned_results[3]), weight_grad)
```

```python
import functools

import jax
import jax.numpy as jnp
from jax import lax
from jax.experimental import pallas as pl
from jax.experimental.pallas import tpu as pltpu
from jax.sharding import PartitionSpec as P

GATE_NORM = 16.0
BF = jnp.bfloat16
F32 = jnp.float32
LANES = 128


def nn(a, b):
    return lax.dot_general(a, b, (((1,), (0,)), ((), ())), preferred_element_type=F32)


def nt(a, b):
    return lax.dot_general(a, b, (((1,), (1,)), ((), ())), preferred_element_type=F32)


def tn(a, b):
    return lax.dot_general(a, b, (((0,), (0,)), ((), ())), preferred_element_type=F32)


def thirds(x, axis):
    top = x.astype(BF)
    rest = x - top.astype(F32)
    middle = rest.astype(BF)
    low = (rest - middle.astype(F32)).astype(BF)
    return jnp.concatenate([top, middle, low], axis=axis)


def kernel(
    n_sp, n_dp,
    q_ref, k_ref, v_ref, do_ref, lat_ref, map_ref, bias_ref, extra_ref,
    dq_ref, dk_ref, dv_ref, lg_ref, wg_ref,
    qd, kd, qs, ke, es, ee, gate, dec, inc, adj, dqi, dki, dvi, rin,
    s_in, s_out, g_in, g_out,
    w_own, a_src, a_dst, b_all, c_all,
    s_send, s_recv, g_send, g_recv, a_send, a_recv, b_send, b_recv, c_send, c_recv,
):
    tokens, width = q_ref.shape
    heads = extra_ref.shape[1]
    key_width = width // heads
    pairs = width // LANES
    value_width = v_ref.shape[1] // pairs
    vd = value_width // 2
    scale = key_width ** (-0.5)
    middle = tokens // 2
    rows = map_ref.shape[0] // n_sp
    me = lax.axis_index("sp")
    mine = lax.axis_index("dp")
    first = me == 0
    last = me == n_sp - 1

    barrier = pltpu.get_barrier_semaphore()
    for o in range(1, n_sp):
        pl.semaphore_signal(barrier, inc=1, device_id={"sp": lax.rem(me + o, n_sp)})
    for o in range(1, n_dp):
        pl.semaphore_signal(barrier, inc=1, device_id={"dp": lax.rem(mine + o, n_dp)})

    row = lax.broadcasted_iota(jnp.int32, (tokens, tokens), 0)
    col = lax.broadcasted_iota(jnp.int32, (tokens, tokens), 1)
    plus = (row >= middle) & (col >= middle) & (col <= row)
    minus = (row < middle) & (col < middle) & (col > row)
    prefix = (plus.astype(F32) - minus.astype(F32)).astype(BF)
    prefix = jnp.concatenate([prefix] * 3, axis=1)
    suffix = (col >= row).astype(F32).astype(BF)
    suffix = jnp.concatenate([suffix] * 3, axis=1)
    causal = jnp.concatenate([col <= row] * 2, axis=1)
    anti = jnp.concatenate([col >= row] * 2, axis=1)
    low_lane = lax.broadcasted_iota(jnp.int32, (tokens, LANES), 1) < key_width
    low_state = lax.broadcasted_iota(jnp.int32, (vd, LANES), 1) < key_width

    def stack(x, low):
        zero = jnp.zeros_like(x)
        return jnp.concatenate([jnp.where(low, x, zero), jnp.where(low, zero, x)], axis=0)

    def lanes(c):
        return slice(c * LANES, (c + 1) * LANES)

    def values(c):
        return slice(c * value_width, (c + 1) * value_width)

    def s_copy(c):
        return pltpu.make_async_remote_copy(
            src_ref=s_out.at[c], dst_ref=s_in.at[c], send_sem=s_send.at[c], recv_sem=s_recv.at[c],
            device_id={"sp": lax.rem(me + 1, n_sp)})

    def g_copy(c):
        return pltpu.make_async_remote_copy(
            src_ref=g_out.at[c], dst_ref=g_in.at[c], send_sem=g_send.at[c], recv_sem=g_recv.at[c],
            device_id={"sp": lax.rem(me + n_sp - 1, n_sp)})

    latent = lat_ref[...]
    extra = extra_ref[...]
    pl.semaphore_wait(barrier, n_sp + n_dp - 2)

    @pl.when(first)
    def _():
        s_in[...] = jnp.zeros_like(s_in)

    @pl.when(last)
    def _():
        g_in[...] = jnp.zeros_like(g_in)

    for c in range(pairs):
        at = lanes(c)
        logit = nn(latent, map_ref[:, at]) + bias_ref[:, at]
        e = jnp.exp(-jnp.abs(logit))
        gate[:, at] = jnp.where(logit >= 0, e, 1.0) / (1.0 + e) / GATE_NORM
        head_of = lax.broadcasted_iota(jnp.int32, (heads, LANES), 1) // key_width + c * (LANES // key_width)
        spread = (lax.broadcasted_iota(jnp.int32, (heads, LANES), 0) == head_of).astype(F32).astype(BF)
        log_decay = (jnp.minimum(logit, 0.0) - jnp.log1p(e)) / GATE_NORM + nn(extra, spread)
        cum = nn(prefix, thirds(log_decay, 0))
        head_total = jnp.sum(log_decay[:middle], axis=0, keepdims=True)
        end = cum[tokens - 1 :]
        dec[:, at] = jnp.exp(head_total + end)
        q = q_ref[:, at].astype(F32) * scale
        k = k_ref[:, at].astype(F32)
        e_start = jnp.exp(cum + head_total)
        e_end = jnp.exp(end - cum)
        es[:, at] = e_start * scale
        ee[:, at] = e_end
        q_start = (q * e_start).astype(BF)
        k_end = (k * e_end).astype(BF)
        qs[:, at] = q_start
        ke[:, at] = k_end
        up = jnp.exp(cum)
        down = jnp.exp(-cum)
        dqi[:, at] = up * scale
        dki[:, at] = down
        qd[:, at] = (q * up).astype(BF)
        kd[:, at] = (k * down).astype(BF)
        both = tn(v_ref[:, values(c)], k_end)
        increment = jnp.where(low_state, both[:vd], both[vd:])
        both = tn(do_ref[:, values(c)], q_start)
        adjoint = jnp.where(low_state, both[:vd], both[vd:])
        inc[c] = increment
        adj[c] = adjoint

        @pl.when(first)
        def _():
            s_out[c] = increment.astype(BF)
            s_copy(c).start()

        @pl.when(last)
        def _():
            g_out[c] = adjoint.astype(BF)
            g_copy(c).start()

    inner = jnp.logical_and(jnp.logical_not(first), jnp.logical_not(last))
    for c in range(pairs):
        at = lanes(c)

        @pl.when(jnp.logical_not(first))
        def _():
            s_copy(c).wait_recv()

        @pl.when(inner)
        def _():
            s_out[c] = (dec[:, at] * s_in[c].astype(F32) + inc[c]).astype(BF)
            s_copy(c).start()

        @pl.when(jnp.logical_not(last))
        def _():
            g_copy(c).wait_recv()

        @pl.when(inner)
        def _():
            g_out[c] = (dec[:, at] * g_in[c].astype(F32) + adj[c]).astype(BF)
            g_copy(c).start()

        qc = qd[:, at]
        kc = kd[:, at]
        q_stack = stack(qc, low_lane)
        k_stack = stack(kc, low_lane)
        v0 = v_ref[:, c * value_width : c * value_width + vd]
        v1 = v_ref[:, c * value_width + vd : (c + 1) * value_width]
        d0 = do_ref[:, c * value_width : c * value_width + vd]
        d1 = do_ref[:, c * value_width + vd : (c + 1) * value_width]
        score_t = jnp.where(anti, nt(kc, q_stack), 0.0).astype(BF)
        a = jnp.where(causal, jnp.concatenate([nt(d0, v0), nt(d1, v1)], axis=1), 0.0).astype(BF)
        a_t = jnp.where(anti, jnp.concatenate([nt(v0, d0), nt(v1, d1)], axis=1), 0.0).astype(BF)
        dq_in = nn(a, k_stack)
        dk_in = nn(a_t, q_stack)
        rin[:, at] = qc.astype(F32) * dq_in - kc.astype(F32) * dk_in
        dqi[:, at] = dqi[:, at] * dq_in
        dki[:, at] = dki[:, at] * dk_in
        dvi[:, values(c)] = jnp.concatenate(
            [nn(score_t[:, :tokens], d0), nn(score_t[:, tokens:], d1)], axis=1)

    latent_total = jnp.zeros((tokens, map_ref.shape[0]), F32)
    for c in range(pairs):
        at = lanes(c)
        state = s_in[c]
        costate = g_in[c]
        g_stack = stack(costate, low_state)
        dq_out = nn(do_ref[:, values(c)], stack(state, low_state))
        dk_out = nn(v_ref[:, values(c)], g_stack)
        dq_ref[:, at] = (dqi[:, at] + es[:, at] * dq_out).astype(BF)
        dk_ref[:, at] = (dki[:, at] + ee[:, at] * dk_out).astype(BF)
        dv_ref[:, values(c)] = (dvi[:, values(c)] + nt(ke[:, at], g_stack)).astype(BF)
        term = rin[:, at] + qs[:, at].astype(F32) * dq_out - ke[:, at].astype(F32) * dk_out
        leaving = dec[:, at] * state.astype(F32) + inc[c]
        carry = jnp.sum(leaving * costate.astype(F32), axis=0, keepdims=True)
        decay_grad = nn(suffix, thirds(term, 0)) + carry
        gate_grad = (decay_grad * gate[:, at]).astype(BF)
        latent_total = latent_total + nt(gate_grad, map_ref[:, at])
        dw = tn(latent, gate_grad)
        for p in range(n_sp):
            piece = dw[p * rows : (p + 1) * rows]
            w_own[p, :, at] = piece
            a_src[p, :, at] = piece.astype(BF)
    lg_ref[...] = latent_total.astype(BF)

    def a_copy(o):
        t = lax.rem(me + o, n_sp)
        return pltpu.make_async_remote_copy(
            src_ref=a_src.at[t], dst_ref=a_dst.at[o], send_sem=a_send.at[o], recv_sem=a_recv.at[o],
            device_id={"sp": t})

    def b_copy(o, slot):
        return pltpu.make_async_remote_copy(
            src_ref=b_all.at[mine], dst_ref=b_all.at[slot], send_sem=b_send.at[o], recv_sem=b_recv.at[o],
            device_id={"dp": lax.rem(mine + o, n_dp)})

    def c_copy(o, slot):
        return pltpu.make_async_remote_copy(
            src_ref=c_all.at[me], dst_ref=c_all.at[slot], send_sem=c_send.at[o], recv_sem=c_recv.at[o],
            device_id={"sp": lax.rem(me + o, n_sp)})

    for o in range(1, n_sp):
        a_copy(o).start()
    total = w_own[me]
    for o in range(1, n_sp):
        a_copy(o).wait_recv()
        total = total + a_dst[o].astype(F32)
    b_all[mine] = total.astype(BF)
    for o in range(1, n_dp):
        b_copy(o, mine).start()
    for o in range(1, n_dp):
        b_copy(o, lax.rem(mine + n_dp - o, n_dp)).wait_recv()
    total = b_all[0].astype(F32)
    for o in range(1, n_dp):
        total = total + b_all[o].astype(F32)
    c_all[me] = total.astype(BF)
    for o in range(1, n_sp):
        c_copy(o, me).start()
    for o in range(1, n_sp):
        c_copy(o, lax.rem(me + n_sp - o, n_sp)).wait_recv()
    for p in range(n_sp):
        wg_ref[p * rows : (p + 1) * rows, :] = c_all[p].astype(F32)

    for c in range(pairs):
        @pl.when(jnp.logical_not(last))
        def _():
            s_copy(c).wait_send()

        @pl.when(jnp.logical_not(first))
        def _():
            g_copy(c).wait_send()

    for o in range(1, n_sp):
        a_copy(o).wait_send()
        c_copy(o, me).wait_send()
    for o in range(1, n_dp):
        b_copy(o, mine).wait_send()


def solution(mesh):
    n_sp = mesh.shape["sp"]
    n_dp = mesh.shape["dp"]

    def on_device(q, k, v, do, latent, weight, bias, extra):
        tokens, width = q.shape
        rank = weight.shape[0]
        pairs = width // LANES
        vd = v.shape[1] // pairs // 2
        rows = rank // n_sp
        vmem = pl.BlockSpec(memory_space=pltpu.VMEM)
        wide = lambda kind: pltpu.VMEM((tokens, width), kind)
        state = lambda kind: pltpu.VMEM((pairs, vd, LANES), kind)
        sems = lambda n: pltpu.SemaphoreType.DMA((n,))
        return pl.pallas_call(
            functools.partial(kernel, n_sp, n_dp),
            out_shape=(
                jax.ShapeDtypeStruct(q.shape, BF),
                jax.ShapeDtypeStruct(k.shape, BF),
                jax.ShapeDtypeStruct(v.shape, BF),
                jax.ShapeDtypeStruct(latent.shape, BF),
                jax.ShapeDtypeStruct(weight.shape, F32),
            ),
            in_specs=[vmem] * 8,
            out_specs=(vmem,) * 5,
            scratch_shapes=[
                wide(BF), wide(BF), wide(BF), wide(BF), wide(F32), wide(F32), wide(F32),
                pltpu.VMEM((1, width), F32), state(F32), state(F32),
                wide(F32), wide(F32), pltpu.VMEM(v.shape, F32), wide(F32),
                state(BF), state(BF), state(BF), state(BF),
                pltpu.VMEM((n_sp, rows, width), F32), pltpu.VMEM((n_sp, rows, width), BF),
                pltpu.VMEM((n_sp, rows, width), BF), pltpu.VMEM((n_dp, rows, width), BF),
                pltpu.VMEM((n_sp, rows, width), BF),
                sems(pairs), sems(pairs), sems(pairs), sems(pairs),
                sems(n_sp), sems(n_sp), sems(n_dp), sems(n_dp), sems(n_sp), sems(n_sp),
            ],
            compiler_params=pltpu.CompilerParams(
                collective_id=0, has_side_effects=True, vmem_limit_bytes=48 * 1024 * 1024),
            name="gla_backward",
        )(q, k, v, do, latent, weight, bias.reshape(1, -1), extra)

    tokens = P(("dp", "sp"), None)
    return jax.shard_map(
        on_device,
        mesh=mesh,
        in_specs=(tokens,) * 5 + (P(), P(), tokens),
        out_specs=(tokens,) * 4 + (P(),),
        check_vma=False,
    )
```

```python
import functools

import jax
import jax.numpy as jnp
from jax import lax
from jax.experimental import pallas as pl
from jax.experimental.pallas import tpu as pltpu
from jax.sharding import PartitionSpec as P

GATE_NORM = 16.0
BF = jnp.bfloat16
F32 = jnp.float32
LANES = 128


def nn(a, b):
    return lax.dot_general(a, b, (((1,), (0,)), ((), ())), preferred_element_type=F32)


def nt(a, b):
    return lax.dot_general(a, b, (((1,), (1,)), ((), ())), preferred_element_type=F32)


def tn(a, b):
    return lax.dot_general(a, b, (((0,), (0,)), ((), ())), preferred_element_type=F32)


def thirds(x, axis):
    top = x.astype(BF)
    rest = x - top.astype(F32)
    middle = rest.astype(BF)
    low = (rest - middle.astype(F32)).astype(BF)
    return jnp.concatenate([top, middle, low], axis=axis)


def kernel(
    n_sp, n_dp,
    q_hbm, k_hbm, v_hbm, do_hbm, lat_hbm, map_hbm, bias_hbm, extra_hbm,
    dq_ref, dk_ref, dv_ref, lg_ref, wg_ref,
    q_ref, k_ref, v_ref, do_ref, lat_ref, map_ref, bias_ref, extra_ref, in_sem,
    qd, kd, qs, ke, es, ee, gate, dec, inc, adj, dqi, dki, dvi, rin,
    s_in, s_out, g_in, g_out,
    w_own, a_src, a_dst, b_all, c_all,
    s_send, s_recv, g_send, g_recv, a_send, a_recv, b_send, b_recv, c_send, c_recv,
):
    tokens, width = q_ref.shape
    heads = extra_ref.shape[0]
    key_width = width // heads
    pairs = width // LANES
    value_width = v_ref.shape[1] // pairs
    vd = value_width // 2
    scale = key_width ** (-0.5)
    middle = tokens // 2
    rows = map_ref.shape[0] // n_sp
    me = lax.axis_index("sp")
    mine = lax.axis_index("dp")
    first = me == 0
    last = me == n_sp - 1

    sources = (lat_hbm, extra_hbm, map_hbm, bias_hbm, k_hbm, q_hbm, v_hbm, do_hbm)
    targets = (lat_ref, extra_ref, map_ref, bias_ref, k_ref, q_ref, v_ref, do_ref)
    loads = [pltpu.make_async_copy(a, b, in_sem.at[n]) for n, (a, b) in enumerate(zip(sources, targets))]
    for load in loads:
        load.start()

    barrier = pltpu.get_barrier_semaphore()
    for o in range(1, n_sp):
        pl.semaphore_signal(barrier, inc=1, device_id={"sp": lax.rem(me + o, n_sp)})
    for o in range(1, n_dp):
        pl.semaphore_signal(barrier, inc=1, device_id={"dp": lax.rem(mine + o, n_dp)})

    row = lax.broadcasted_iota(jnp.int32, (tokens, tokens), 0)
    col = lax.broadcasted_iota(jnp.int32, (tokens, tokens), 1)
    plus = (row >= middle) & (col >= middle) & (col <= row)
    minus = (row < middle) & (col < middle) & (col > row)
    prefix = (plus.astype(F32) - minus.astype(F32)).astype(BF)
    prefix = jnp.concatenate([prefix] * 3, axis=1)
    suffix = (col >= row).astype(F32).astype(BF)
    suffix = jnp.concatenate([suffix] * 3, axis=1)
    causal = jnp.concatenate([col <= row] * 2, axis=1)
    anti = jnp.concatenate([col >= row] * 2, axis=1)
    low_lane = lax.broadcasted_iota(jnp.int32, (tokens, LANES), 1) < key_width
    low_state = lax.broadcasted_iota(jnp.int32, (vd, LANES), 1) < key_width

    def stack(x, low):
        zero = jnp.zeros_like(x)
        return jnp.concatenate([jnp.where(low, x, zero), jnp.where(low, zero, x)], axis=0)

    def lanes(c):
        return slice(c * LANES, (c + 1) * LANES)

    def values(c):
        return slice(c * value_width, (c + 1) * value_width)

    def s_copy(c):
        return pltpu.make_async_remote_copy(
            src_ref=s_out.at[c], dst_ref=s_in.at[c], send_sem=s_send.at[c], recv_sem=s_recv.at[c],
            device_id={"sp": lax.rem(me + 1, n_sp)})

    def g_copy(c):
        return pltpu.make_async_remote_copy(
            src_ref=g_out.at[c], dst_ref=g_in.at[c], send_sem=g_send.at[c], recv_sem=g_recv.at[c],
            device_id={"sp": lax.rem(me + n_sp - 1, n_sp)})

    for load in loads:
        load.wait()
    latent_t = lat_ref[...]
    latent = latent_t.astype(F32).T.astype(BF)
    extra = extra_ref[...].astype(F32).T.astype(BF)
    pl.semaphore_wait(barrier, n_sp + n_dp - 2)

    @pl.when(first)
    def _():
        s_in[...] = jnp.zeros_like(s_in)

    @pl.when(last)
    def _():
        g_in[...] = jnp.zeros_like(g_in)

    for c in range(pairs):
        at = lanes(c)
        logit = nn(latent, map_ref[:, at]) + bias_ref[:, at]
        e = jnp.exp(-jnp.abs(logit))
        gate[:, at] = jnp.where(logit >= 0, e, 1.0) / (1.0 + e) / GATE_NORM
        head_of = lax.broadcasted_iota(jnp.int32, (heads, LANES), 1) // key_width + c * (LANES // key_width)
        spread = (lax.broadcasted_iota(jnp.int32, (heads, LANES), 0) == head_of).astype(F32).astype(BF)
        log_decay = (jnp.minimum(logit, 0.0) - jnp.log1p(e)) / GATE_NORM + nn(extra, spread)
        cum = nn(prefix, thirds(log_decay, 0))
        head_total = jnp.sum(log_decay[:middle], axis=0, keepdims=True)
        end = cum[tokens - 1 :]
        dec[:, at] = jnp.exp(head_total + end)
        q = q_ref[:, at].astype(F32) * scale
        k = k_ref[:, at].astype(F32)
        e_start = jnp.exp(cum + head_total)
        e_end = jnp.exp(end - cum)
        es[:, at] = e_start * scale
        ee[:, at] = e_end
        q_start = (q * e_start).astype(BF)
        k_end = (k * e_end).astype(BF)
        qs[:, at] = q_start
        ke[:, at] = k_end
        up = jnp.exp(cum)
        down = jnp.exp(-cum)
        dqi[:, at] = up * scale
        dki[:, at] = down
        qd[:, at] = (q * up).astype(BF)
        kd[:, at] = (k * down).astype(BF)
        both = tn(v_ref[:, values(c)], k_end)
        increment = jnp.where(low_state, both[:vd], both[vd:])
        both = tn(do_ref[:, values(c)], q_start)
        adjoint = jnp.where(low_state, both[:vd], both[vd:])
        inc[c] = increment
        adj[c] = adjoint

        @pl.when(first)
        def _():
            s_out[c] = increment.astype(BF)
            s_copy(c).start()

        @pl.when(last)
        def _():
            g_out[c] = adjoint.astype(BF)
            g_copy(c).start()

    def relay_s(c):
        s_copy(c).wait_recv()

        @pl.when(jnp.logical_not(last))
        def _():
            s_out[c] = (dec[:, lanes(c)] * s_in[c].astype(F32) + inc[c]).astype(BF)
            s_copy(c).start()

    def relay_g(c):
        g_copy(c).wait_recv()

        @pl.when(jnp.logical_not(first))
        def _():
            g_out[c] = (dec[:, lanes(c)] * g_in[c].astype(F32) + adj[c]).astype(BF)
            g_copy(c).start()

    def inside(c):
        at = lanes(c)
        qc = qd[:, at]
        kc = kd[:, at]
        q_stack = stack(qc, low_lane)
        k_stack = stack(kc, low_lane)
        v0 = v_ref[:, c * value_width : c * value_width + vd]
        v1 = v_ref[:, c * value_width + vd : (c + 1) * value_width]
        d0 = do_ref[:, c * value_width : c * value_width + vd]
        d1 = do_ref[:, c * value_width + vd : (c + 1) * value_width]
        score_t = jnp.where(anti, nt(kc, q_stack), 0.0).astype(BF)
        a = jnp.where(causal, jnp.concatenate([nt(d0, v0), nt(d1, v1)], axis=1), 0.0).astype(BF)
        a_t = jnp.where(anti, jnp.concatenate([nt(v0, d0), nt(v1, d1)], axis=1), 0.0).astype(BF)
        dq_in = nn(a, k_stack)
        dk_in = nn(a_t, q_stack)
        rin[:, at] = qc.astype(F32) * dq_in - kc.astype(F32) * dk_in
        dqi[:, at] = dqi[:, at] * dq_in
        dki[:, at] = dki[:, at] * dk_in
        dvi[:, values(c)] = jnp.concatenate(
            [nn(score_t[:, :tokens], d0), nn(score_t[:, tokens:], d1)], axis=1)

    lead = pairs // 2
    left = me < n_sp // 2
    for c in range(lead):
        inside(c)
    for step in range(pairs + lead):
        if step < pairs:
            @pl.when(jnp.logical_and(left, jnp.logical_not(first)))
            def _():
                relay_s(step)

            @pl.when(jnp.logical_not(jnp.logical_or(left, last)))
            def _():
                relay_g(step)

            if step >= lead:
                inside(step)
        if step >= lead:
            @pl.when(left)
            def _():
                relay_g(step - lead)

            @pl.when(jnp.logical_not(left))
            def _():
                relay_s(step - lead)

    latent_total = jnp.zeros((map_ref.shape[0], tokens), F32)
    for c in range(pairs):
        at = lanes(c)
        state = s_in[c]
        costate = g_in[c]
        g_stack = stack(costate, low_state)
        dq_out = nn(do_ref[:, values(c)], stack(state, low_state))
        dk_out = nn(v_ref[:, values(c)], g_stack)
        dq_ref[:, at] = (dqi[:, at] + es[:, at] * dq_out).astype(BF)
        dk_ref[:, at] = (dki[:, at] + ee[:, at] * dk_out).astype(BF)
        dv_ref[:, values(c)] = (dvi[:, values(c)] + nt(ke[:, at], g_stack)).astype(BF)
        term = rin[:, at] + qs[:, at].astype(F32) * dq_out - ke[:, at].astype(F32) * dk_out
        leaving = dec[:, at] * state.astype(F32) + inc[c]
        carry = jnp.sum(leaving * costate.astype(F32), axis=0, keepdims=True)
        decay_grad = nn(suffix, thirds(term, 0)) + carry
        gate_grad = (decay_grad * gate[:, at]).astype(BF)
        latent_total = latent_total + nt(map_ref[:, at], gate_grad)
        dw = nn(latent_t, gate_grad)
        for p in range(n_sp):
            piece = dw[p * rows : (p + 1) * rows]
            w_own[p, :, at] = piece
            a_src[p, :, at] = piece.astype(BF)
    lg_ref[...] = latent_total.astype(BF)

    def a_copy(o):
        t = lax.rem(me + o, n_sp)
        return pltpu.make_async_remote_copy(
            src_ref=a_src.at[t], dst_ref=a_dst.at[o], send_sem=a_send.at[o], recv_sem=a_recv.at[o],
            device_id={"sp": t})

    def b_copy(o, slot):
        return pltpu.make_async_remote_copy(
            src_ref=b_all.at[mine], dst_ref=b_all.at[slot], send_sem=b_send.at[o], recv_sem=b_recv.at[o],
            device_id={"dp": lax.rem(mine + o, n_dp)})

    def c_copy(o, slot):
        return pltpu.make_async_remote_copy(
            src_ref=c_all.at[me], dst_ref=c_all.at[slot], send_sem=c_send.at[o], recv_sem=c_recv.at[o],
            device_id={"sp": lax.rem(me + o, n_sp)})

    for o in range(1, n_sp):
        a_copy(o).start()
    total = w_own[me]
    for o in range(1, n_sp):
        a_copy(o).wait_recv()
        total = total + a_dst[o].astype(F32)
    b_all[mine] = total.astype(BF)
    for o in range(1, n_dp):
        b_copy(o, mine).start()
    for o in range(1, n_dp):
        b_copy(o, lax.rem(mine + n_dp - o, n_dp)).wait_recv()
    total = b_all[0].astype(F32)
    for o in range(1, n_dp):
        total = total + b_all[o].astype(F32)
    c_all[me] = total.astype(BF)
    for o in range(1, n_sp):
        c_copy(o, me).start()
    for o in range(1, n_sp):
        c_copy(o, lax.rem(me + n_sp - o, n_sp)).wait_recv()
    for p in range(n_sp):
        wg_ref[p * rows : (p + 1) * rows, :] = c_all[p].astype(F32)

    for c in range(pairs):
        @pl.when(jnp.logical_not(last))
        def _():
            s_copy(c).wait_send()

        @pl.when(jnp.logical_not(first))
        def _():
            g_copy(c).wait_send()

    for o in range(1, n_sp):
        a_copy(o).wait_send()
        c_copy(o, me).wait_send()
    for o in range(1, n_dp):
        b_copy(o, mine).wait_send()


def solution(mesh):
    n_sp = mesh.shape["sp"]
    n_dp = mesh.shape["dp"]

    def on_device(q, k, v, do, latent, weight, bias, extra):
        tokens, width = q.shape
        rank = weight.shape[0]
        pairs = width // LANES
        vd = v.shape[1] // pairs // 2
        rows = rank // n_sp
        vmem = pl.BlockSpec(memory_space=pltpu.VMEM)
        wide = lambda kind: pltpu.VMEM((tokens, width), kind)
        state = lambda kind: pltpu.VMEM((pairs, vd, LANES), kind)
        sems = lambda n: pltpu.SemaphoreType.DMA((n,))
        grads = pl.pallas_call(
            functools.partial(kernel, n_sp, n_dp),
            out_shape=(
                jax.ShapeDtypeStruct(q.shape, BF),
                jax.ShapeDtypeStruct(k.shape, BF),
                jax.ShapeDtypeStruct(v.shape, BF),
                jax.ShapeDtypeStruct(latent.shape[::-1], BF),
                jax.ShapeDtypeStruct(weight.shape, F32),
            ),
            in_specs=[pl.BlockSpec(memory_space=pltpu.HBM)] * 8,
            out_specs=(vmem,) * 5,
            scratch_shapes=[
                pltpu.VMEM(q.shape, BF), pltpu.VMEM(k.shape, BF), pltpu.VMEM(v.shape, BF), pltpu.VMEM(do.shape, BF),
                pltpu.VMEM(latent.shape[::-1], BF), pltpu.VMEM(weight.shape, BF),
                pltpu.VMEM((1, width), F32), pltpu.VMEM(extra.shape[::-1], BF), sems(8),
                wide(BF), wide(BF), wide(BF), wide(BF), wide(F32), wide(F32), wide(F32),
                pltpu.VMEM((1, width), F32), state(F32), state(F32),
                wide(F32), wide(F32), pltpu.VMEM(v.shape, F32), wide(F32),
                state(BF), state(BF), state(BF), state(BF),
                pltpu.VMEM((n_sp, rows, width), F32), pltpu.VMEM((n_sp, rows, width), BF),
                pltpu.VMEM((n_sp, rows, width), BF), pltpu.VMEM((n_dp, rows, width), BF),
                pltpu.VMEM((n_sp, rows, width), BF),
                sems(pairs), sems(pairs), sems(pairs), sems(pairs),
                sems(n_sp), sems(n_sp), sems(n_dp), sems(n_dp), sems(n_sp), sems(n_sp),
            ],
            compiler_params=pltpu.CompilerParams(
                collective_id=0, has_side_effects=True, vmem_limit_bytes=48 * 1024 * 1024),
            name="gla_backward",
        )(q, k, v, do, latent.T, weight, bias.reshape(1, -1), extra.T)
        return grads[0], grads[1], grads[2], grads[3].T, grads[4]

    tokens = P(("dp", "sp"), None)
    return jax.shard_map(
        on_device,
        mesh=mesh,
        in_specs=(tokens,) * 5 + (P(), P(), tokens),
        out_specs=(tokens,) * 4 + (P(),),
        check_vma=False,
    )
```

```python
import functools

import jax
import jax.numpy as jnp
from jax import lax
from jax.experimental import pallas as pl
from jax.experimental.pallas import tpu as pltpu
from jax.sharding import PartitionSpec as P

GATE_NORM = 16.0
BF = jnp.bfloat16
F32 = jnp.float32
LANES = 128
HALVES = 2


def nn(a, b):
    return lax.dot_general(a, b, (((1,), (0,)), ((), ())), preferred_element_type=F32)


def nt(a, b):
    return lax.dot_general(a, b, (((1,), (1,)), ((), ())), preferred_element_type=F32)


def tn(a, b):
    return lax.dot_general(a, b, (((0,), (0,)), ((), ())), preferred_element_type=F32)


def thirds(x, axis):
    top = x.astype(BF)
    rest = x - top.astype(F32)
    middle = rest.astype(BF)
    low = (rest - middle.astype(F32)).astype(BF)
    return jnp.concatenate([top, middle, low], axis=axis)


def kernel(
    n_sp, n_dp,
    q_hbm, k_hbm, v_hbm, do_hbm, lat_hbm, map_hbm, bias_hbm, extra_hbm,
    dq_ref, dk_ref, dv_ref, lg_ref, wg_ref,
    q_ref, k_ref, v_ref, do_ref, lat_ref, map_ref, bias_ref, extra_ref, in_sem,
    qd, kd, qs, ke, es, ee, gate, dec, inc, adj, dqi, dki, dvi, rin,
    s_in, s_out, g_in, g_out,
    w_own, a_src, a_dst, b_all, c_all,
    s_send, s_recv, g_send, g_recv, a_send, a_recv, b_send, b_recv, c_send, c_recv,
):
    tokens, width = q_ref.shape
    heads = extra_ref.shape[0]
    key_width = width // heads
    pairs = width // LANES
    value_width = v_ref.shape[1] // pairs
    vd = value_width // 2
    scale = key_width ** (-0.5)
    middle = tokens // 2
    rows = map_ref.shape[0] // n_sp
    me = lax.axis_index("sp")
    mine = lax.axis_index("dp")
    first = me == 0
    last = me == n_sp - 1

    sources = (lat_hbm, extra_hbm, map_hbm, bias_hbm, k_hbm, q_hbm, v_hbm, do_hbm)
    targets = (lat_ref, extra_ref, map_ref, bias_ref, k_ref, q_ref, v_ref, do_ref)
    loads = [pltpu.make_async_copy(a, b, in_sem.at[n]) for n, (a, b) in enumerate(zip(sources, targets))]
    for load in loads:
        load.start()

    barrier = pltpu.get_barrier_semaphore()
    for o in range(1, n_sp):
        pl.semaphore_signal(barrier, inc=1, device_id={"sp": lax.rem(me + o, n_sp)})
    for o in range(1, n_dp):
        pl.semaphore_signal(barrier, inc=1, device_id={"dp": lax.rem(mine + o, n_dp)})

    row = lax.broadcasted_iota(jnp.int32, (tokens, tokens), 0)
    col = lax.broadcasted_iota(jnp.int32, (tokens, tokens), 1)
    plus = (row >= middle) & (col >= middle) & (col <= row)
    minus = (row < middle) & (col < middle) & (col > row)
    prefix = (plus.astype(F32) - minus.astype(F32)).astype(BF)
    prefix = jnp.concatenate([prefix] * 3, axis=1)
    suffix = (col >= row).astype(F32).astype(BF)
    suffix = jnp.concatenate([suffix] * 3, axis=1)
    causal = jnp.concatenate([col <= row] * 2, axis=1)
    anti = jnp.concatenate([col >= row] * 2, axis=1)
    low_lane = lax.broadcasted_iota(jnp.int32, (tokens, LANES), 1) < key_width
    low_state = lax.broadcasted_iota(jnp.int32, (vd, LANES), 1) < key_width

    def stack(x, low):
        zero = jnp.zeros_like(x)
        return jnp.concatenate([jnp.where(low, x, zero), jnp.where(low, zero, x)], axis=0)

    def lanes(c):
        return slice(c * LANES, (c + 1) * LANES)

    def values(c):
        return slice(c * value_width, (c + 1) * value_width)

    def s_copy(c):
        return pltpu.make_async_remote_copy(
            src_ref=s_out.at[c], dst_ref=s_in.at[c], send_sem=s_send.at[c], recv_sem=s_recv.at[c],
            device_id={"sp": lax.rem(me + 1, n_sp)})

    def g_copy(c):
        return pltpu.make_async_remote_copy(
            src_ref=g_out.at[c], dst_ref=g_in.at[c], send_sem=g_send.at[c], recv_sem=g_recv.at[c],
            device_id={"sp": lax.rem(me + n_sp - 1, n_sp)})

    for load in loads:
        load.wait()
    latent_t = lat_ref[...]
    latent = latent_t.astype(F32).T.astype(BF)
    extra = extra_ref[...].astype(F32).T.astype(BF)

    @pl.when(first)
    def _():
        s_in[...] = jnp.zeros_like(s_in)

    @pl.when(last)
    def _():
        g_in[...] = jnp.zeros_like(g_in)

    for c in range(pairs):
        at = lanes(c)
        logit = nn(latent, map_ref[:, at]) + bias_ref[:, at]
        e = jnp.exp(-jnp.abs(logit))
        gate[:, at] = jnp.where(logit >= 0, e, 1.0) / (1.0 + e) / GATE_NORM
        head_of = lax.broadcasted_iota(jnp.int32, (heads, LANES), 1) // key_width + c * (LANES // key_width)
        spread = (lax.broadcasted_iota(jnp.int32, (heads, LANES), 0) == head_of).astype(F32).astype(BF)
        log_decay = (jnp.minimum(logit, 0.0) - jnp.log1p(e)) / GATE_NORM + nn(extra, spread)
        cum = nn(prefix, thirds(log_decay, 0))
        head_total = jnp.sum(log_decay[:middle], axis=0, keepdims=True)
        end = cum[tokens - 1 :]
        dec[:, at] = jnp.exp(head_total + end)
        q = q_ref[:, at].astype(F32) * scale
        k = k_ref[:, at].astype(F32)
        e_start = jnp.exp(cum + head_total)
        e_end = jnp.exp(end - cum)
        es[:, at] = e_start * scale
        ee[:, at] = e_end
        q_start = (q * e_start).astype(BF)
        k_end = (k * e_end).astype(BF)
        qs[:, at] = q_start
        ke[:, at] = k_end
        up = jnp.exp(cum)
        down = jnp.exp(-cum)
        dqi[:, at] = up * scale
        dki[:, at] = down
        qd[:, at] = (q * up).astype(BF)
        kd[:, at] = (k * down).astype(BF)
        both = tn(v_ref[:, values(c)], k_end)
        increment = jnp.where(low_state, both[:vd], both[vd:])
        both = tn(do_ref[:, values(c)], q_start)
        adjoint = jnp.where(low_state, both[:vd], both[vd:])
        inc[c] = increment
        adj[c] = adjoint
        if c == 0:
            pl.semaphore_wait(barrier, n_sp + n_dp - 2)

        @pl.when(first)
        def _():
            s_out[c] = increment.astype(BF)
            s_copy(c).start()

        @pl.when(last)
        def _():
            g_out[c] = adjoint.astype(BF)
            g_copy(c).start()

    def relay_s(c):
        s_copy(c).wait_recv()

        @pl.when(jnp.logical_not(last))
        def _():
            s_out[c] = (dec[:, lanes(c)] * s_in[c].astype(F32) + inc[c]).astype(BF)
            s_copy(c).start()

    def relay_g(c):
        g_copy(c).wait_recv()

        @pl.when(jnp.logical_not(first))
        def _():
            g_out[c] = (dec[:, lanes(c)] * g_in[c].astype(F32) + adj[c]).astype(BF)
            g_copy(c).start()

    def inside(c):
        at = lanes(c)
        qc = qd[:, at]
        kc = kd[:, at]
        q_stack = stack(qc, low_lane)
        k_stack = stack(kc, low_lane)
        v0 = v_ref[:, c * value_width : c * value_width + vd]
        v1 = v_ref[:, c * value_width + vd : (c + 1) * value_width]
        d0 = do_ref[:, c * value_width : c * value_width + vd]
        d1 = do_ref[:, c * value_width + vd : (c + 1) * value_width]
        score_t = jnp.where(anti, nt(kc, q_stack), 0.0).astype(BF)
        a = jnp.where(causal, jnp.concatenate([nt(d0, v0), nt(d1, v1)], axis=1), 0.0).astype(BF)
        a_t = jnp.where(anti, jnp.concatenate([nt(v0, d0), nt(v1, d1)], axis=1), 0.0).astype(BF)
        dq_in = nn(a, k_stack)
        dk_in = nn(a_t, q_stack)
        rin[:, at] = qc.astype(F32) * dq_in - kc.astype(F32) * dk_in
        dqi[:, at] = dqi[:, at] * dq_in
        dki[:, at] = dki[:, at] * dk_in
        dvi[:, values(c)] = jnp.concatenate(
            [nn(score_t[:, :tokens], d0), nn(score_t[:, tokens:], d1)], axis=1)

    lead = pairs // HALVES

    def a_copy(h, o):
        t = lax.rem(me + o, n_sp)
        return pltpu.make_async_remote_copy(
            src_ref=a_src.at[h, t], dst_ref=a_dst.at[h, o], send_sem=a_send.at[h, o],
            recv_sem=a_recv.at[h, o], device_id={"sp": t})

    def b_copy(h, o, slot):
        return pltpu.make_async_remote_copy(
            src_ref=b_all.at[h, mine], dst_ref=b_all.at[h, slot], send_sem=b_send.at[h, o],
            recv_sem=b_recv.at[h, o], device_id={"dp": lax.rem(mine + o, n_dp)})

    def c_copy(h, o, slot):
        return pltpu.make_async_remote_copy(
            src_ref=c_all.at[h, me], dst_ref=c_all.at[h, slot], send_sem=c_send.at[h, o],
            recv_sem=c_recv.at[h, o], device_id={"sp": lax.rem(me + o, n_sp)})


    latent_parts = []

    def final(c):
        at = lanes(c)
        here = lanes(c % lead)
        state = s_in[c]
        costate = g_in[c]
        g_stack = stack(costate, low_state)
        dq_out = nn(do_ref[:, values(c)], stack(state, low_state))
        dk_out = nn(v_ref[:, values(c)], g_stack)
        dq_ref[:, at] = (dqi[:, at] + es[:, at] * dq_out).astype(BF)
        dk_ref[:, at] = (dki[:, at] + ee[:, at] * dk_out).astype(BF)
        dv_ref[:, values(c)] = (dvi[:, values(c)] + nt(ke[:, at], g_stack)).astype(BF)
        term = rin[:, at] + qs[:, at].astype(F32) * dq_out - ke[:, at].astype(F32) * dk_out
        leaving = dec[:, at] * state.astype(F32) + inc[c]
        carry = jnp.sum(leaving * costate.astype(F32), axis=0, keepdims=True)
        decay_grad = nn(suffix, thirds(term, 0)) + carry
        gate_grad = (decay_grad * gate[:, at]).astype(BF)
        latent_parts.append(nt(map_ref[:, at], gate_grad))
        dw = nn(latent_t, gate_grad)
        for p in range(n_sp):
            piece = dw[p * rows : (p + 1) * rows]
            w_own[c // lead, p, :, here] = piece
            a_src[c // lead, p, :, here] = piece.astype(BF)

    left = me < n_sp // 2
    for c in range(lead):
        inside(c)
    for step in range(pairs + lead):
        if step < pairs:
            @pl.when(jnp.logical_and(left, jnp.logical_not(first)))
            def _():
                relay_s(step)

            @pl.when(jnp.logical_not(jnp.logical_or(left, last)))
            def _():
                relay_g(step)

            if step >= lead:
                inside(step)
        if step >= lead:
            @pl.when(left)
            def _():
                relay_g(step - lead)

            @pl.when(jnp.logical_not(left))
            def _():
                relay_s(step - lead)

            final(step - lead)
            if (step + 1) % lead == 0:
                for o in range(1, n_sp):
                    a_copy(step // lead - 1, o).start()

    lg_ref[...] = functools.reduce(jnp.add, latent_parts).astype(BF)

    halves = range(HALVES)
    for h in halves:
        total = w_own[h, me]
        for o in range(1, n_sp):
            a_copy(h, o).wait_recv()
            total = total + a_dst[h, o].astype(F32)
        b_all[h, mine] = total.astype(BF)
        for o in range(1, n_dp):
            b_copy(h, o, mine).start()
    for h in halves:
        for o in range(1, n_dp):
            b_copy(h, o, lax.rem(mine + n_dp - o, n_dp)).wait_recv()
        total = b_all[h, 0].astype(F32)
        for o in range(1, n_dp):
            total = total + b_all[h, o].astype(F32)
        c_all[h, me] = total.astype(BF)
        for o in range(1, n_sp):
            c_copy(h, o, me).start()
    for h in halves:
        for o in range(1, n_sp):
            c_copy(h, o, lax.rem(me + n_sp - o, n_sp)).wait_recv()
        half = wg_ref.shape[1] // HALVES
        for p in range(n_sp):
            wg_ref[p * rows : (p + 1) * rows, h * half : (h + 1) * half] = c_all[h, p].astype(F32)

    for c in range(pairs):
        @pl.when(jnp.logical_not(last))
        def _():
            s_copy(c).wait_send()

        @pl.when(jnp.logical_not(first))
        def _():
            g_copy(c).wait_send()

    for h in halves:
        for o in range(1, n_sp):
            a_copy(h, o).wait_send()
            c_copy(h, o, me).wait_send()
        for o in range(1, n_dp):
            b_copy(h, o, mine).wait_send()


def writer(*refs):
    n = len(refs) // 2
    sem = refs[-1]
    copies = [pltpu.make_async_copy(a, b, sem.at[i]) for i, (a, b) in enumerate(zip(refs[:n], refs[n:-1]))]
    for copy in copies:
        copy.start()
    for copy in copies:
        copy.wait()


def write_out(arrays):
    hbm = pl.BlockSpec(memory_space=pltpu.HBM)
    return pl.pallas_call(
        writer,
        out_shape=tuple(jax.ShapeDtypeStruct(a.shape, a.dtype) for a in arrays),
        in_specs=[pl.BlockSpec(memory_space=pltpu.VMEM)] * len(arrays),
        out_specs=(hbm,) * len(arrays),
        scratch_shapes=[pltpu.SemaphoreType.DMA((len(arrays),))],
        name="write_out",
    )(*arrays)


def solution(mesh):
    n_sp = mesh.shape["sp"]
    n_dp = mesh.shape["dp"]

    def on_device(q, k, v, do, latent, weight, bias, extra):
        tokens, width = q.shape
        rank = weight.shape[0]
        pairs = width // LANES
        vd = v.shape[1] // pairs // 2
        rows = rank // n_sp
        vmem = pl.BlockSpec(memory_space=pltpu.VMEM)
        wide = lambda kind: pltpu.VMEM((tokens, width), kind)
        state = lambda kind: pltpu.VMEM((pairs, vd, LANES), kind)
        sems = lambda n: pltpu.SemaphoreType.DMA((n,))
        halves = lambda n: pltpu.SemaphoreType.DMA((HALVES, n))
        grads = pl.pallas_call(
            functools.partial(kernel, n_sp, n_dp),
            out_shape=(
                jax.ShapeDtypeStruct(q.shape, BF),
                jax.ShapeDtypeStruct(k.shape, BF),
                jax.ShapeDtypeStruct(v.shape, BF),
                jax.ShapeDtypeStruct(latent.shape[::-1], BF),
                jax.ShapeDtypeStruct(weight.shape, F32),
            ),
            in_specs=[pl.BlockSpec(memory_space=pltpu.HBM)] * 8,
            out_specs=(vmem,) * 5,
            scratch_shapes=[
                pltpu.VMEM(q.shape, BF), pltpu.VMEM(k.shape, BF), pltpu.VMEM(v.shape, BF), pltpu.VMEM(do.shape, BF),
                pltpu.VMEM(latent.shape[::-1], BF), pltpu.VMEM(weight.shape, BF),
                pltpu.VMEM((1, width), F32), pltpu.VMEM(extra.shape[::-1], BF), sems(8),
                wide(BF), wide(BF), wide(BF), wide(BF), wide(F32), wide(F32), wide(F32),
                pltpu.VMEM((1, width), F32), state(F32), state(F32),
                wide(F32), wide(F32), pltpu.VMEM(v.shape, F32), wide(F32),
                state(BF), state(BF), state(BF), state(BF),
                pltpu.VMEM((HALVES, n_sp, rows, width // HALVES), F32), pltpu.VMEM((HALVES, n_sp, rows, width // HALVES), BF),
                pltpu.VMEM((HALVES, n_sp, rows, width // HALVES), BF), pltpu.VMEM((HALVES, n_dp, rows, width // HALVES), BF),
                pltpu.VMEM((HALVES, n_sp, rows, width // HALVES), BF),
                sems(pairs), sems(pairs), sems(pairs), sems(pairs),
                halves(n_sp), halves(n_sp), halves(n_dp), halves(n_dp), halves(n_sp), halves(n_sp),
            ],
            compiler_params=pltpu.CompilerParams(
                collective_id=0, has_side_effects=True, vmem_limit_bytes=67043328),
            name="gla_backward",
        )(q, k, v, do, latent.T, weight, bias.reshape(1, -1), extra.T)
        grads = write_out(grads)
        return grads[0], grads[1], grads[2], grads[3].T, grads[4]

    tokens = P(("dp", "sp"), None)
    return jax.shard_map(
        on_device,
        mesh=mesh,
        in_specs=(tokens,) * 5 + (P(), P(), tokens),
        out_specs=(tokens,) * 4 + (P(),),
        check_vma=False,
    )
```
